32 devices in a mesh: grp: 2 (over y), fs: 4 (over z), tp: 4 (over x, core).
Axes of the slice: x: 2, y: 2, z: 4, core: 2. Of those that a mesh axis runs over, the one named last changes fastest.
Arguments:
- tokens: bfloat16 [2048, 2048], P(('grp', 'fs')), parts along dimension 0, may hold values from -6 to 6
- route_ids: int32 [2048, 2], P(('grp', 'fs')), parts along dimension 0, may hold values from 0 to 7, as said below
- route_weights: float32 [2048, 2], P(('grp', 'fs')), parts along dimension 0, may hold values from 0.2 to 1
- ffn_gain: float32 [2048], P('fs'), may hold values from 0.1 to 1.9
- gate_master: float32 [8, 2048, 1024], P(None, 'fs', 'tp'), may hold values from -0.125 to 0.125
- up_master: float32 [8, 2048, 1024], P(None, 'fs', 'tp'), may hold values from -0.125 to 0.125
- down_master: float32 [8, 1024, 2048], P(None, 'fs', 'tp'), may hold values from -0.1875 to 0.1875
Outputs:
- gate_serve: bfloat16 [16, 2048, 1024], P(('grp', 'fs'), None, 'tp'), parts along dimension 0
- up_serve: bfloat16 [16, 2048, 1024], P(('grp', 'fs'), None, 'tp'), parts along dimension 0
- down_serve: bfloat16 [16, 1024, 2048], P(('grp', 'fs'), None, 'tp'), parts along dimension 0
- mixed: bfloat16 [2048, 2048], P(('grp', 'fs'), 'tp'), parts along dimension 0
The draws below stay inside these ranges and needn't reach their ends.
There are 2 independent parts, one for each index of `grp`. The reference program is written for one: setup_inputs(seed, part) draws one part's arguments, and reference() takes and returns one part's arrays. A program takes and returns all parts, laid end to end along the dimension named above; an argument that names none is the same for every part. Nothing has to cross between parts.
Inputs may be any that keep to these rules, and one draw needn't show every extreme that they name: `route_ids`: each row names two different experts of one group of 8 consecutive experts. Among the tokens of one index of fs, each group is named by exactly 256 tokens and no expert by more than 128; in every group one expert, the same for every index of fs, is named by exactly 128, and so is one other expert of the group, which may change from one index of fs to the next.
All inputs are finite; a program needn't handle non-finite values.
Results may differ from the reference program's by a relative error of at most 0.0087.
Values may be sent and summed in bfloat16 or wider, within the bound.
A program may use at most 64 MiB of HBM per device.

```python
import jax
import jax.numpy as jnp
from jax import lax

D = 2048
FF = 1024
GROUP_SIZE = 8
TOK_DEV = 256
EXPERTS = 8
GROUPS = 1
CAP = 128
TOKENS = 1024
N_FS = 4


def draw_route_ids(key, part):
    blocks = TOKENS // TOK_DEV
    per_group = TOK_DEV // GROUPS
    half_group = per_group // 2
    others_count = GROUP_SIZE - 2
    hot_local = jax.random.randint(jax.random.fold_in(key, 11), (GROUPS,), 0, GROUP_SIZE).astype(jnp.int32)
    rank_list = jnp.arange(TOK_DEV, dtype=jnp.int32)
    group_of = rank_list // per_group
    within = rank_list % per_group
    leading = within < half_group
    local_list = jnp.arange(GROUP_SIZE, dtype=jnp.int32)
    block_keys = jax.random.split(jax.random.fold_in(key, 13), blocks)
    block_list = jnp.arange(blocks, dtype=jnp.int32)

    def one_block(subkey, block_index):
        step_draw = jax.random.randint(jax.random.fold_in(subkey, 4), (GROUPS,), 0, GROUP_SIZE - 1).astype(jnp.int32)
        drawn_second = (hot_local + 1 + step_draw) % GROUP_SIZE
        paired = jnp.bitwise_xor(hot_local, 1)
        second_full = jnp.where(block_index % 2 == 0, paired, drawn_second)
        group_keys = jax.random.split(jax.random.fold_in(subkey, 3), GROUPS)
        ranks = jax.vmap(lambda inner_key: jax.random.permutation(inner_key, GROUP_SIZE))(group_keys).astype(jnp.int32)
        excluded = (local_list[None, :] == hot_local[:, None]) | (local_list[None, :] == second_full[:, None])
        scores = ranks + GROUP_SIZE * excluded.astype(jnp.int32)
        ordered = jnp.argsort(scores, axis=1).astype(jnp.int32)
        others = ordered[:, :others_count]
        first_local = jnp.where(leading, hot_local[group_of], second_full[group_of])
        second_local = others[group_of, within % others_count]
        pairing = jnp.stack([first_local, second_local], axis=1) + group_of[:, None] * GROUP_SIZE
        placing = jax.random.permutation(jax.random.fold_in(subkey, 1), TOK_DEV)
        flipped = jax.random.randint(jax.random.fold_in(subkey, 2), (TOK_DEV, 1), 0, 2)
        swapped = jnp.where(flipped == 1, pairing[:, ::-1], pairing)
        return jnp.zeros((TOK_DEV, 2), jnp.int32).at[placing].set(swapped.astype(jnp.int32))
    return jax.vmap(one_block)(block_keys, block_list).reshape(TOKENS, 2).astype(jnp.int32)


def shard_levels(key, extent, cuts, low, largest):
    def one(axis_at, shards_of):
        heights = jax.random.uniform(jax.random.fold_in(jax.random.fold_in(key, 6), axis_at), (shards_of,), jnp.float32, low / len(cuts), largest / len(cuts))
        return jnp.repeat(jnp.exp(heights), extent[axis_at] // shards_of).reshape((-1,) + (1,) * (len(extent) - axis_at - 1))

    factor_of = one(*cuts[0])
    for cut in cuts[1:]:
        factor_of = factor_of * one(*cut)
    return factor_of


def normal_values(key, dims, scale, limit, cuts=(), held_as=jnp.bfloat16):
    entries = jax.random.normal(key, dims, jnp.float32) * scale
    if len(cuts) > 0:
        entries = shard_levels(key, dims, cuts, -0.22, 0.18) * entries
    return jnp.clip(entries, min=-limit, max=limit).astype(held_as)


def setup_inputs(seed: int = 0, part: int = 0) -> dict:
    key_list = jax.random.split(jax.random.key(seed), 8)
    part_splits = jax.random.split(jax.random.fold_in(key_list[7], part), 8)
    tokens = normal_values(part_splits[0], (TOKENS, D), 1.0, 6.0, ((0, 4),))
    route_ids = draw_route_ids(jax.random.fold_in(jax.random.fold_in(key_list[7], part), 71), part)
    route_weights = jnp.clip(0.2 + 0.8 * jax.random.uniform(part_splits[2], (TOKENS, 2), jnp.float32) ** shard_levels(part_splits[2], (TOKENS, 2), ((0, 4),), -0.2, 0.2), 0.2, 1.0)
    ffn_gain = jnp.clip(1.0 + 0.18 * jax.random.normal(key_list[3], (D,), jnp.float32), 0.1, 1.9)
    gate_master = normal_values(key_list[4], (EXPERTS, D, FF), D ** -0.5, 0.125, ((1, 4), (2, 4)), jnp.float32)
    up_master = normal_values(key_list[5], (EXPERTS, D, FF), D ** -0.5, 0.125, ((1, 4), (2, 4)), jnp.float32)
    down_master = normal_values(key_list[6], (EXPERTS, FF, D), FF ** -0.5, 0.1875, ((1, 4), (2, 4)), jnp.float32)
    return {"tokens": tokens, "route_ids": route_ids, "route_weights": route_weights, "ffn_gain": ffn_gain, "gate_master": gate_master, "up_master": up_master, "down_master": down_master}


def reference(tokens, route_ids, route_weights, ffn_gain, gate_master, up_master, down_master):
    row_gain = ffn_gain.astype(jnp.float32)[None, :, None]
    gate_serve = (gate_master * row_gain).astype(jnp.bfloat16)
    up_serve = (up_master * row_gain).astype(jnp.bfloat16)
    down_serve = down_master.astype(jnp.bfloat16)
    token_rows = tokens.astype(jnp.float32)
    normed = (token_rows * lax.rsqrt(lax.optimization_barrier(jnp.mean(token_rows * token_rows, axis=1, keepdims=True)) + 1e-06)).astype(jnp.bfloat16)
    flat_ids = route_ids.reshape(-1).astype(jnp.int32)
    flat_weights = route_weights.reshape(-1).astype(jnp.float32)
    slot_limit = N_FS * CAP

    def one_expert(inputs):
        expert, w_gate, w_up, w_down = inputs
        matches = flat_ids == expert
        chosen = jnp.nonzero(matches, size=slot_limit, fill_value=0)[0].astype(jnp.int32)
        live_count = jnp.sum(matches.astype(jnp.int32))
        is_live = jnp.arange(slot_limit, dtype=jnp.int32) < live_count
        picked = normed[chosen // 2]
        gate_val = jnp.dot(picked, w_gate, preferred_element_type=jnp.float32)
        up_val = jnp.dot(picked, w_up, preferred_element_type=jnp.float32)
        hidden = (jax.nn.silu(gate_val) * up_val).astype(jnp.bfloat16)
        route_out = jnp.dot(hidden, w_down, preferred_element_type=jnp.float32).astype(jnp.bfloat16)
        route_scale = jnp.where(is_live, flat_weights[chosen], jnp.zeros_like(flat_weights[chosen]))
        return (chosen // 2, route_out.astype(jnp.float32) * route_scale[:, None])
    expert_list = jnp.arange(gate_serve.shape[0], dtype=jnp.int32)
    owners, terms = lax.map(one_expert, (expert_list, gate_serve, up_serve, down_serve))
    combined = jnp.zeros(tokens.shape, jnp.float32).at[owners.reshape(-1)].add(terms.reshape(-1, tokens.shape[1]))
    return (gate_serve, up_serve, down_serve, combined.astype(jnp.bfloat16))
```

```python
import functools

import jax
import jax.numpy as jnp
from jax import lax
from jax.experimental import pallas as pl
from jax.experimental.pallas import tpu as pltpu
from jax.sharding import PartitionSpec as P

GROUP_SIZE = 8
MESH = pl.DeviceIdType.MESH


def slot_targets(route_ids, experts, capacity):
    flat_ids = route_ids.reshape(-1)
    member = (flat_ids[:, None] == jnp.arange(experts, dtype=jnp.int32)[None, :]).astype(jnp.int32)
    before = jnp.cumsum(member, axis=0) - member
    slot_index = jnp.sum(before * member, axis=1)
    return flat_ids * capacity + slot_index


def kernel(
    G, N, T, cap,
    tok_ref, meta_ref, gain_ref, gate_hbm, up_hbm, down_hbm,
    gs_ref, us_ref, ds_ref, mixed_ref,
    gate_f, up_f, down_f, stage_gu, stage_d, tok_all, meta_all, x_buf, hid_all, part_send, part_recv,
    load_sem, ts, tr, ms, mr, xs, xr, zs, zr, ys, yr, hs, hr, ps, pr,
):
    g, z, t = lax.axis_index("grp"), lax.axis_index("fs"), lax.axis_index("tp")
    E, R, C = gate_f.shape
    Ed = E // N
    tokens, Dq = tok_ref.shape[1:]
    FFq = C
    masters, serves = (gate_f, up_f, down_f), (gs_ref, us_ref, ds_ref)
    rows = (R, R, down_f.shape[1])

    loads = [
        pltpu.make_async_copy(src, dst, load_sem.at[w])
        for w, (src, dst) in enumerate(zip((gate_hbm, up_hbm, down_hbm), masters))
    ]
    for load in loads:
        load.start()

    barrier = pltpu.get_barrier_semaphore()
    for axis, me, size in (("grp", g, G), ("fs", z, N), ("tp", t, T)):
        for k in range(1, size):
            pl.semaphore_signal(barrier, inc=1, device_id={axis: lax.rem(me + k, size)}, device_id_type=MESH)
    pl.semaphore_wait(barrier, G + N + T - 3)

    def remote(src, dst, send, recv, axis, peer):
        copy = pltpu.make_async_remote_copy(
            src_ref=src, dst_ref=dst, send_sem=send, recv_sem=recv, device_id={axis: peer}, device_id_type=MESH
        )
        copy.start()
        return copy

    sent = []
    tok_copies, meta_copies = {}, {}
    for k in range(1, N):
        peer = lax.rem(z + k, N)
        meta_copies[k] = remote(meta_ref, meta_all.at[z], ms.at[k], mr.at[k], "fs", peer)
        tok_copies[k] = remote(tok_ref.at[t], tok_all.at[z, t], ts.at[k], tr.at[k], "fs", peer)

    z_copies = {}

    def send_weights(w):
        loads[w].wait()
        sub = rows[w] // G
        start = pl.multiple_of(g * sub, sub)
        for k in range(1, N):
            peer = lax.rem(z + k, N)
            stage = stage_d.at[k] if w == 2 else stage_gu.at[w, k]
            for e in range(Ed):
                block = masters[w][peer * Ed + e, pl.ds(start, sub), :]
                if w < 2:
                    block = block * gain_ref[pl.ds(start, sub), :]
                stage[e] = block.astype(jnp.bfloat16)
            where = pl.multiple_of(z * rows[w] + start, sub)
            z_copies[w, k] = remote(
                stage, serves[w].at[:, pl.ds(where, sub), :], zs.at[w, k], zr.at[w, k], "fs", peer
            )

    def keep_own(w):
        where = pl.multiple_of(z * rows[w], rows[w])
        for e in range(Ed):
            block = masters[w][z * Ed + e]
            if w < 2:
                block = block * gain_ref[...]
            serves[w][e, pl.ds(where, rows[w]), :] = block.astype(jnp.bfloat16)

    y_copies = []

    def relay_weights(w):
        sub = rows[w] // G
        for k in range(1, N):
            z_copies[w, k].wait_recv()
            origin = lax.rem(z + N - k, N)
            where = pl.multiple_of(origin * rows[w] + g * sub, sub)
            view = serves[w].at[:, pl.ds(where, sub), :]
            for j in range(1, G):
                y_copies.append(
                    (w, remote(view, view, ys.at[w, k, j], yr.at[w, k, j], "grp", lax.rem(g + j, G)))
                )

    def finish_weights(w):
        for which, copy in y_copies:
            if which == w:
                copy.wait_recv()

    send_weights(0)
    send_weights(1)
    send_weights(2)

    meta_all[z] = meta_ref[...]
    tok_all[z] = tok_ref[...]
    for w in range(3):
        keep_own(w)

    x_copies = []
    for k in range(1, N):
        tok_copies[k].wait_recv()
        origin = lax.rem(z + N - k, N)
        view = tok_all.at[origin, t]
        for j in range(1, T):
            x_copies.append(remote(view, view, xs.at[k, j], xr.at[k, j], "tp", lax.rem(t + j, T)))
    for k in range(1, N):
        meta_copies[k].wait_recv()
    relay_weights(0)
    for copy in x_copies:
        copy.wait_recv()

    SB = Ed * cap
    base = (z * SB).astype(jnp.float32)

    def hits(n):
        slot = lax.broadcasted_iota(jnp.int32, (SB, tokens), 0).astype(jnp.float32) + base
        info = meta_all[n]
        return info[0:1, :] == slot, info[1:2, :] == slot, info

    def dispatch(n, carry):
        first, second, _ = hits(n)
        pick = (first.astype(jnp.float32) + second.astype(jnp.float32)).astype(jnp.bfloat16)
        for q in range(T):
            got = jnp.dot(pick, tok_all[n, q], preferred_element_type=jnp.float32).astype(jnp.bfloat16)
            for e in range(Ed):
                x_buf[e, pl.ds(pl.multiple_of(n * cap, cap), cap), q * Dq:(q + 1) * Dq] = got[e * cap:(e + 1) * cap]
        return carry

    lax.fori_loop(0, N, dispatch, 0)
    relay_weights(1)
    finish_weights(0)
    finish_weights(1)

    def experts_in(i, carry):
        e = i // N
        at = pl.ds(pl.multiple_of((i % N) * cap, cap), cap)
        x = x_buf[e, at, :]
        gate = jnp.dot(x, gs_ref[e], preferred_element_type=jnp.float32)
        up = jnp.dot(x, us_ref[e], preferred_element_type=jnp.float32)
        hid_all[t, e, at, :] = (gate / (1.0 + jnp.exp(-gate)) * up).astype(jnp.bfloat16)
        return carry

    lax.fori_loop(0, Ed * N, experts_in, 0)
    h_copies = []
    for j in range(1, T):
        view = hid_all.at[t]
        h_copies.append(remote(view, view, hs.at[j], hr.at[j], "tp", lax.rem(t + j, T)))
    relay_weights(2)
    finish_weights(2)
    for copy in h_copies:
        copy.wait_recv()

    def partial_rows(n):
        first, second, info = hits(n)
        weight = jnp.sum(
            jnp.where(first, info[2:3, :], 0.0) + jnp.where(second, info[3:4, :], 0.0), axis=1, keepdims=True
        )
        pick = (first.astype(jnp.float32) + second.astype(jnp.float32)).astype(jnp.bfloat16)
        at = pl.ds(pl.multiple_of(n * cap, cap), cap)
        outs = []
        for e in range(Ed):
            out = jnp.zeros((cap, ds_ref.shape[2]), jnp.float32)
            for q in range(T):
                out += jnp.dot(
                    hid_all[q, e, at, :], ds_ref[e, q * FFq:(q + 1) * FFq, :], preferred_element_type=jnp.float32
                )
            outs.append(out.astype(jnp.bfloat16).astype(jnp.float32))
        scaled = (jnp.concatenate(outs, axis=0) * weight).astype(jnp.bfloat16)
        return lax.dot_general(pick, scaled, (((0,), (0,)), ((), ())), preferred_element_type=jnp.float32)

    p_copies = []
    for k in range(1, N):
        peer = lax.rem(z + k, N)
        part_send[k] = partial_rows(peer).astype(jnp.bfloat16)
        p_copies.append(remote(part_send.at[k], part_recv.at[k], ps.at[k], pr.at[k], "fs", peer))
    total = partial_rows(z)
    for copy in p_copies:
        copy.wait_recv()
    for k in range(1, N):
        total += part_recv[k].astype(jnp.float32)
    mixed_ref[...] = total.astype(jnp.bfloat16)

    for copy in (
        list(tok_copies.values()) + list(meta_copies.values()) + list(z_copies.values())
        + [c for _, c in y_copies] + x_copies + h_copies + p_copies
    ):
        copy.wait_send()


def on_device(G, N, T, tokens, route_ids, route_weights, ffn_gain, gate_master, up_master, down_master):
    experts, R, C = gate_master.shape
    R2, C2 = down_master.shape[1:]
    count, D = tokens.shape
    Ed = experts // N
    capacity = count // (2 * (experts // GROUP_SIZE))
    token_rows = tokens.astype(jnp.float32)
    normed = (
        token_rows * lax.rsqrt(jnp.mean(token_rows * token_rows, axis=1, keepdims=True) + 1e-06)
    ).astype(jnp.bfloat16)
    Dq = D // T
    quarters = normed.reshape(count, T, Dq).transpose(1, 0, 2)
    targets = slot_targets(route_ids, experts, capacity).reshape(count, 2)
    meta = jnp.concatenate(
        [targets.T.astype(jnp.float32), route_weights.T, jnp.zeros((4, count), jnp.float32)], axis=0
    )
    bf = jnp.bfloat16
    vmem = pl.BlockSpec(memory_space=pltpu.VMEM)
    anyspace = pl.BlockSpec(memory_space=pl.ANY)
    slots = N * capacity
    dma = pltpu.SemaphoreType.DMA
    return pl.pallas_call(
        functools.partial(kernel, G, N, T, capacity),
        out_shape=(
            jax.ShapeDtypeStruct((Ed, N * R, C), bf),
            jax.ShapeDtypeStruct((Ed, N * R, C), bf),
            jax.ShapeDtypeStruct((Ed, N * R2, C2), bf),
            jax.ShapeDtypeStruct((count, C2), bf),
        ),
        in_specs=[vmem, vmem, vmem, anyspace, anyspace, anyspace],
        out_specs=(vmem, vmem, vmem, vmem),
        scratch_shapes=[
            pltpu.VMEM((experts, R, C), jnp.float32),
            pltpu.VMEM((experts, R, C), jnp.float32),
            pltpu.VMEM((experts, R2, C2), jnp.float32),
            pltpu.VMEM((2, N, Ed, R // G, C), bf),
            pltpu.VMEM((N, Ed, R2 // G, C2), bf),
            pltpu.VMEM((N, T, count, Dq), bf),
            pltpu.VMEM((N, 8, count), jnp.float32),
            pltpu.VMEM((Ed, slots, D), bf),
            pltpu.VMEM((T, Ed, slots, C), bf),
            pltpu.VMEM((N, count, C2), bf),
            pltpu.VMEM((N, count, C2), bf),
            dma((3,)),
            dma((N,)), dma((N,)), dma((N,)), dma((N,)),
            dma((N, T)), dma((N, T)),
            dma((3, N)), dma((3, N)),
            dma((3, N, G)), dma((3, N, G)),
            dma((T,)), dma((T,)),
            dma((N,)), dma((N,)),
        ],
        compiler_params=pltpu.CompilerParams(
            collective_id=0, has_side_effects=True, vmem_limit_bytes=63 * 1024 * 1024
        ),
    )(quarters, meta, ffn_gain.reshape(R, 1), gate_master, up_master, down_master)


def solution(mesh):
    in_specs = (
        P(("grp", "fs"), None),
        P(("grp", "fs"), None),
        P(("grp", "fs"), None),
        P("fs"),
        P(None, "fs", "tp"),
        P(None, "fs", "tp"),
        P(None, "fs", "tp"),
    )
    out_specs = (
        P(("grp", "fs"), None, "tp"),
        P(("grp", "fs"), None, "tp"),
        P(("grp", "fs"), None, "tp"),
        P(("grp", "fs"), "tp"),
    )
    body = functools.partial(on_device, mesh.shape["grp"], mesh.shape["fs"], mesh.shape["tp"])
    return jax.shard_map(body, mesh=mesh, in_specs=in_specs, out_specs=out_specs, check_vma=False)
```

```python
import functools

import jax
import jax.numpy as jnp
from jax import lax
from jax.experimental import pallas as pl
from jax.experimental.pallas import tpu as pltpu
from jax.sharding import PartitionSpec as P

GROUP_SIZE = 8
MESH = pl.DeviceIdType.MESH


def kernel(
    G, N, T, cap,
    tok_ref, ids_ref, weights_ref, gain_ref, gate_hbm, up_hbm, down_hbm,
    gate_out, up_out, down_out, mixed_ref,
    gate_f, up_f, down_f, gs_ref, us_ref, ds_ref, gain_col, meta_ref, stage_gu, stage_d, tok_all, meta_all,
    x_buf, hid_all, ret_send, ret_recv, total_ref,
    load_sem, out_sem, ts, tr, ms, mr, xs, xr, zs, zr, ys, yr, hs, hr, ps, pr,
):
    g, z, t = lax.axis_index("grp"), lax.axis_index("fs"), lax.axis_index("tp")
    E, R, C = gate_f.shape
    Ed = E // N
    tokens, D = tok_ref.shape
    Dq = D // T
    masters, serves = (gate_f, up_f, down_f), (gs_ref, us_ref, ds_ref)
    outs = (gate_out, up_out, down_out)
    rows = (R, R, down_f.shape[1])

    loads = [
        pltpu.make_async_copy(src, dst, load_sem.at[w])
        for w, (src, dst) in enumerate(zip((gate_hbm, up_hbm, down_hbm), masters))
    ]
    for load in loads:
        load.start()

    barrier = pltpu.get_barrier_semaphore()
    for axis, me, size in (("grp", g, G), ("fs", z, N), ("tp", t, T)):
        for k in range(1, size):
            pl.semaphore_signal(barrier, inc=1, device_id={axis: lax.rem(me + k, size)}, device_id_type=MESH)

    def normalize(c, carry):
        at = pl.ds(pl.multiple_of(c * 32, 32), 32)
        wide = tok_ref[at, :].astype(jnp.float32)
        unit = (wide * lax.rsqrt(jnp.mean(wide * wide, axis=1, keepdims=True) + 1e-06)).astype(jnp.bfloat16)
        for q in range(T):
            tok_all[z, q, at, :] = unit[:, q * Dq:(q + 1) * Dq]
        return carry

    lax.fori_loop(0, tokens // 32, normalize, 0)

    expert_of = lax.broadcasted_iota(jnp.int32, (E, tokens), 0)
    named = [ids_ref[r:r + 1, :] == expert_of for r in range(2)]
    member = (named[0].astype(jnp.float32) + named[1].astype(jnp.float32)).astype(jnp.bfloat16)
    earlier = (
        lax.broadcasted_iota(jnp.int32, (tokens, tokens), 0) < lax.broadcasted_iota(jnp.int32, (tokens, tokens), 1)
    ).astype(jnp.float32).astype(jnp.bfloat16)
    place = jnp.dot(member, earlier, preferred_element_type=jnp.float32) + (expert_of * cap).astype(jnp.float32)
    meta_ref[...] = jnp.zeros_like(meta_ref)
    for r in range(2):
        meta_ref[r:r + 1, :] = jnp.sum(jnp.where(named[r], place, 0.0), axis=0, keepdims=True)
    meta_ref[2:4, :] = weights_ref[...]

    pl.semaphore_wait(barrier, G + N + T - 3)

    def describe(src, dst, send, recv, axis, peer):
        return pltpu.make_async_remote_copy(
            src_ref=src, dst_ref=dst, send_sem=send, recv_sem=recv, device_id={axis: peer}, device_id_type=MESH
        )

    def remote(*args):
        copy = describe(*args)
        copy.start()
        return copy

    def along(way):
        return z + (1 - 2 * way)

    def exists(way):
        return z < N - 1 if way == 0 else z > 0

    def reached(way, d):
        return z >= d if way == 0 else z + d < N

    def tok_step(way, d):
        origin = z - d if way == 0 else z + d
        view = tok_all.at[origin, t]
        return describe(view, view, ts.at[way, d], tr.at[way, d + 1], "fs", along(way))

    def tok_arrival(way, d):
        view = tok_all.at[z, t]
        return describe(view, view, ts.at[way, d - 1], tr.at[way, d], "fs", along(way))

    def tok_share(way, d, j):
        origin = z - d if way == 0 else z + d
        view = tok_all.at[origin, t]
        return describe(view, view, xs.at[way, d, j], xr.at[way, d, j], "tp", lax.rem(t + j, T))

    def each_way(d, condition, action):
        for way in range(2):
            pl.when(condition(way, d))(functools.partial(action, way, d))

    def can_pass(way, d):
        return exists(way) if d == 0 else jnp.logical_and(reached(way, d), exists(way))

    def pass_tokens(d):
        def arrive(way, d):
            tok_arrival(way, d).wait_recv()
            for j in range(1, T):
                tok_share(way, d, j).start()

        if d > 0:
            each_way(d, reached, arrive)
        if d < N - 1:
            each_way(d, can_pass, lambda way, d: tok_step(way, d).start())

    pass_tokens(0)
    meta_copies = {}
    for k in range(1, N):
        meta_copies[k] = remote(meta_ref, meta_all.at[z], ms.at[k], mr.at[k], "fs", lax.rem(z + k, N))

    square = (R, R)
    eye = lax.broadcasted_iota(jnp.int32, square, 0) == lax.broadcasted_iota(jnp.int32, square, 1)
    gain_col[...] = jnp.sum(jnp.where(eye, gain_ref[...], 0.0), axis=1, keepdims=True)

    z_copies = {}

    def send_weights(w, e):
        sub = rows[w] // G
        start = pl.multiple_of(g * sub, sub)
        where = pl.multiple_of(z * rows[w] + start, sub)
        for k in range(1, N):
            peer = lax.rem(z + k, N)
            stage = stage_d.at[e, k] if w == 2 else stage_gu.at[w, e, k]
            block = masters[w][peer * Ed + e, pl.ds(start, sub), :]
            if w < 2:
                block = block * gain_col[pl.ds(start, sub), :]
            stage[...] = block.astype(jnp.bfloat16)
            z_copies[w, e, k] = remote(
                stage, serves[w].at[e, pl.ds(where, sub), :], zs.at[w, e, k], zr.at[w, e, k], "fs", peer
            )

    def keep_own(w, e):
        where = pl.multiple_of(z * rows[w], rows[w])
        block = masters[w][z * Ed + e]
        if w < 2:
            block = block * gain_col[...]
        serves[w][e, pl.ds(where, rows[w]), :] = block.astype(jnp.bfloat16)

    y_copies, out_copies = {}, []

    def relay_weights(w, e):
        sub = rows[w] // G
        for k in range(1, N):
            z_copies[w, e, k].wait_recv()
            origin = lax.rem(z + N - k, N)
            where = pl.multiple_of(origin * rows[w] + g * sub, sub)
            view = serves[w].at[e, pl.ds(where, sub), :]
            for j in range(1, G):
                y_copies[w, e, k, j] = remote(
                    view, view, ys.at[w, e, k, j], yr.at[w, e, k, j], "grp", lax.rem(g + j, G)
                )

    def finish_weights(w, e):
        for k in range(1, N):
            for j in range(1, G):
                y_copies[w, e, k, j].wait_recv()
        copy = pltpu.make_async_copy(serves[w].at[e], outs[w].at[e], out_sem.at[w, e])
        copy.start()
        out_copies.append(copy)

    passed = 0
    for e in range(Ed):
        for w in range(3):
            if e == 0:
                loads[w].wait()
            send_weights(w, e)
            if passed < N - 1:
                passed += 1
                pass_tokens(passed)
    for d in range(passed + 1, N):
        pass_tokens(d)
    meta_all[z] = meta_ref[...]
    for e in range(Ed):
        for w in range(3):
            keep_own(w, e)
    for k in range(1, N):
        meta_copies[k].wait_recv()

    def hits(info, base):
        slot = lax.broadcasted_iota(jnp.int32, (cap, tokens), 0).astype(jnp.float32) + (base * cap).astype(jnp.float32)
        first, second = info[0:1, :] == slot, info[1:2, :] == slot
        return first, second, (first.astype(jnp.float32) + second.astype(jnp.float32)).astype(jnp.bfloat16)

    def dispatch(n, carry):
        info = meta_all[n]
        pick = jnp.concatenate([hits(info, z * Ed + e)[2].astype(jnp.float32) for e in range(Ed)], axis=0)
        pick = pick.astype(jnp.bfloat16)
        for q in range(T):
            got = jnp.dot(pick, tok_all[n, q], preferred_element_type=jnp.float32).astype(jnp.bfloat16)
            for e in range(Ed):
                x_buf[e, pl.ds(pl.multiple_of(n * cap, cap), cap), q * Dq:(q + 1) * Dq] = got[e * cap:(e + 1) * cap]
        return carry

    h_copies, p_copies = {}, {}

    def experts_in(e):
        def block(n, carry):
            at = pl.ds(pl.multiple_of(n * cap, cap), cap)
            x = x_buf[e, at, :]
            gate = jnp.dot(x, gs_ref[e], preferred_element_type=jnp.float32)
            up = jnp.dot(x, us_ref[e], preferred_element_type=jnp.float32)
            hid_all[t, e, at, :] = (gate / (1.0 + jnp.exp(-gate)) * up).astype(jnp.bfloat16)
            return carry

        lax.fori_loop(0, N, block, 0)
        view = hid_all.at[t, e]
        for j in range(1, T):
            h_copies[e, j] = remote(view, view, hs.at[e, j], hr.at[e, j], "tp", lax.rem(t + j, T))

    def experts_out(e):
        for j in range(1, T):
            h_copies[e, j].wait_recv()
        for k in list(range(1, N)) + [0]:
            peer = lax.rem(z + k, N)
            info = meta_all[peer]
            first, second, _ = hits(info, z * Ed + e)
            weight = jnp.sum(
                jnp.where(first, info[2:3, :], 0.0) + jnp.where(second, info[3:4, :], 0.0), axis=1, keepdims=True
            )
            at = pl.ds(pl.multiple_of(peer * cap, cap), cap)
            out = jnp.zeros((cap, ds_ref.shape[2]), jnp.float32)
            for q in range(T):
                out += jnp.dot(
                    hid_all[q, e, at, :], ds_ref[e, q * C:(q + 1) * C, :], preferred_element_type=jnp.float32
                )
            scaled = (out.astype(jnp.bfloat16).astype(jnp.float32) * weight).astype(jnp.bfloat16)
            if k == 0:
                ret_recv[e, 0] = scaled
            else:
                ret_send[e, k] = scaled
                p_copies[e, k] = remote(
                    ret_send.at[e, k], ret_recv.at[e, k], ps.at[e, k], pr.at[e, k], "fs", peer
                )

    def combine(e):
        info = meta_ref[...]
        for k in range(N):
            if k > 0:
                p_copies[e, k].wait_recv()
            pick = hits(info, lax.rem(z + N - k, N) * Ed + e)[2]
            part = lax.dot_general(
                pick, ret_recv[e, k], (((0,), (0,)), ((), ())), preferred_element_type=jnp.float32
            )
            if e == 0 and k == 0:
                total_ref[...] = part
            else:
                total_ref[...] += part

    for e in range(Ed):
        relay_weights(0, e)
        relay_weights(1, e)
        if e == 0:
            for d in range(1, N):
                each_way(d, reached, lambda way, d: [tok_share(way, d, j).wait_recv() for j in range(1, T)] and None)
            lax.fori_loop(0, N, dispatch, 0)
        finish_weights(0, e)
        finish_weights(1, e)
        experts_in(e)
        relay_weights(2, e)
        finish_weights(2, e)
        experts_out(e)
    for e in range(Ed):
        combine(e)
    mixed_ref[...] = total_ref[...].astype(jnp.bfloat16)

    for d in range(N - 1):
        each_way(d, can_pass, lambda way, d: tok_step(way, d).wait_send())
    for d in range(1, N):
        each_way(d, reached, lambda way, d: [tok_share(way, d, j).wait_send() for j in range(1, T)] and None)
    for group in (meta_copies, z_copies, y_copies, h_copies, p_copies):
        for copy in group.values():
            copy.wait_send()
    for copy in out_copies:
        copy.wait()


def on_device(G, N, T, tokens, route_ids, route_weights, ffn_gain, gate_master, up_master, down_master):
    experts, R, C = gate_master.shape
    R2, C2 = down_master.shape[1:]
    count, D = tokens.shape
    Ed = experts // N
    capacity = count // (2 * (experts // GROUP_SIZE))
    Dq = D // T
    bf = jnp.bfloat16
    vmem = pl.BlockSpec(memory_space=pltpu.VMEM)
    anyspace = pl.BlockSpec(memory_space=pl.ANY)
    slots = N * capacity
    dma = pltpu.SemaphoreType.DMA
    return pl.pallas_call(
        functools.partial(kernel, G, N, T, capacity),
        out_shape=(
            jax.ShapeDtypeStruct((Ed, N * R, C), bf),
            jax.ShapeDtypeStruct((Ed, N * R, C), bf),
            jax.ShapeDtypeStruct((Ed, N * R2, C2), bf),
            jax.ShapeDtypeStruct((count, C2), bf),
        ),
        in_specs=[vmem, vmem, vmem, vmem, anyspace, anyspace, anyspace],
        out_specs=(anyspace, anyspace, anyspace, vmem),
        scratch_shapes=[
            pltpu.VMEM((experts, R, C), jnp.float32),
            pltpu.VMEM((experts, R, C), jnp.float32),
            pltpu.VMEM((experts, R2, C2), jnp.float32),
            pltpu.VMEM((Ed, N * R, C), bf),
            pltpu.VMEM((Ed, N * R, C), bf),
            pltpu.VMEM((Ed, N * R2, C2), bf),
            pltpu.VMEM((R, 1), jnp.float32),
            pltpu.VMEM((8, count), jnp.float32),
            pltpu.VMEM((2, Ed, N, R // G, C), bf),
            pltpu.VMEM((Ed, N, R2 // G, C2), bf),
            pltpu.VMEM((N, T, count, Dq), bf),
            pltpu.VMEM((N, 8, count), jnp.float32),
            pltpu.VMEM((Ed, slots, D), bf),
            pltpu.VMEM((T, Ed, slots, C), bf),
            pltpu.VMEM((Ed, N, capacity, C2), bf),
            pltpu.VMEM((Ed, N, capacity, C2), bf),
            pltpu.VMEM((count, C2), jnp.float32),
            dma((3,)), dma((3, Ed)),
            dma((2, N)), dma((2, N)), dma((N,)), dma((N,)),
            dma((2, N, T)), dma((2, N, T)),
            dma((3, Ed, N)), dma((3, Ed, N)),
            dma((3, Ed, N, G)), dma((3, Ed, N, G)),
            dma((Ed, T)), dma((Ed, T)),
            dma((Ed, N)), dma((Ed, N)),
        ],
        compiler_params=pltpu.CompilerParams(
            collective_id=0, has_side_effects=True, vmem_limit_bytes=63 * 1024 * 1024
        ),
    )(tokens, route_ids.T, route_weights.T, ffn_gain.reshape(1, R), gate_master, up_master, down_master)


def solution(mesh):
    in_specs = (
        P(("grp", "fs"), None),
        P(("grp", "fs"), None),
        P(("grp", "fs"), None),
        P("fs"),
        P(None, "fs", "tp"),
        P(None, "fs", "tp"),
        P(None, "fs", "tp"),
    )
    out_specs = (
        P(("grp", "fs"), None, "tp"),
        P(("grp", "fs"), None, "tp"),
        P(("grp", "fs"), None, "tp"),
        P(("grp", "fs"), "tp"),
    )
    body = functools.partial(on_device, mesh.shape["grp"], mesh.shape["fs"], mesh.shape["tp"])
    return jax.shard_map(body, mesh=mesh, in_specs=in_specs, out_specs=out_specs, check_vma=False)
```
